32 devices in a mesh: rep: 4 (over z), fs: 4 (over y, x), tp: 2 (over core).
Axes of the slice: x: 2, y: 2, z: 4, core: 2. Of those that a mesh axis runs over, the one named last changes fastest.
Arguments:
- inputs: bfloat16 [4096, 2048], P(('rep', 'fs', 'tp')), may hold values from -6 to 6
- out_grad: bfloat16 [4096, 2048], P(('rep', 'fs', 'tp')), may hold values from -6 to 6
- pre_act: bfloat16 [4096, 8192], P('rep', ('fs', 'tp')), may hold values from -6 to 6
- w_up: bfloat16 [2048, 8192], P('rep', ('fs', 'tp')), may hold values from -0.125 to 0.125
- w_down_t: bfloat16 [2048, 8192], P('rep', ('fs', 'tp')), may hold values from -0.0625 to 0.0625
Outputs:
- grad_in: bfloat16 [4096, 2048], P(('rep', 'fs', 'tp'))
- grad_up: float32 [2048, 8192], P('rep', ('fs', 'tp'))
- grad_down_t: float32 [2048, 8192], P('rep', ('fs', 'tp'))
The draws below stay inside these ranges and needn't reach their ends.
All inputs are finite; a program needn't handle non-finite values.
Results may differ from the reference program's by a relative error of at most 0.014.
Values may be sent and summed in bfloat16 or wider, within the bound.
A program may use at most 128 MiB of HBM per device.

```python
import jax
import jax.numpy as jnp
from jax import lax

D = 2048
FF = 8192
TOKENS = 4096
N_FS = 4
N_TP = 2


def with_spikes(entries, rng, source, target, shards_of, factor):
    owner, partner = [(jnp.arange(entries.shape[position]) // (entries.shape[position] // shards_of)).reshape([-1 if axis == position else 1 for axis in range(entries.ndim)]) for position in (source, target)]
    chosen = jax.random.permutation(rng, shards_of)[partner]
    strong = (owner == chosen) | (owner == (partner + shards_of // 2) % shards_of)
    return jnp.where(strong, factor * entries, entries)


def shard_levels(own_key, dims, cuts, low, top_value):
    level, own = 1.0, jax.random.fold_in(own_key, 6)
    for dim, shards_of in cuts:
        draws = jnp.exp(jax.random.uniform(jax.random.fold_in(own, dim), (shards_of,), jnp.float32, low / len(cuts), top_value / len(cuts)))
        level = level * jnp.repeat(draws, dims[dim] // shards_of).reshape([-1 if axis == dim else 1 for axis in range(len(dims))])
    return level


def noise(rng, extent, scale, most, cuts=(), dtype=jnp.bfloat16):
    factor_of = shard_levels(rng, extent, cuts, -0.22, 0.18) if cuts else 1.0
    values = jax.random.normal(rng, extent, jnp.float32) * scale * factor_of
    return jnp.minimum(jnp.maximum(values, -most), most).astype(dtype)


def noise_with(own_key, dims, spread, reach, pieces, heavy, kind=jnp.bfloat16):
    result = spread * jax.random.normal(own_key, dims, jnp.float32)
    if pieces:
        result = result * shard_levels(own_key, dims, pieces, -0.22, 0.18)
    return jnp.clip(with_spikes(result, jax.random.fold_in(own_key, 3), *heavy), -reach, reach).astype(kind)


def setup_inputs(seed: int = 0) -> dict:
    arg_keys = jax.random.split(jax.random.key(seed), 6)
    inputs = noise(arg_keys[0], (TOKENS, D), 1.0, 6.0, ((0, 32),))
    out_grad = noise_with(arg_keys[1], (TOKENS, D), 1.0, 6.0, ((0, 32),), (0, 1, 32, 2.75))
    pre_act = noise(arg_keys[2], (TOKENS, FF), 1.0, 6.0, ((0, 4), (1, 8)))
    w_up = noise(arg_keys[3], (D, FF), D ** -0.5, 0.125, ((0, 4), (1, 8)))
    w_down_t = noise(arg_keys[4], (D, FF), FF ** -0.5, 0.0625, ((0, 4), (1, 8)))
    return {"inputs": inputs, "out_grad": out_grad, "pre_act": pre_act, "w_up": w_up, "w_down_t": w_down_t}


def reference(inputs, out_grad, pre_act, w_up, w_down_t):
    pre_float = pre_act.astype(jnp.float32)
    linear = jnp.maximum(pre_float, 0.0)
    squared = (linear * linear).astype(jnp.bfloat16)
    grad_squared = jnp.dot(out_grad, w_down_t, preferred_element_type=jnp.float32)
    grad_pre = (grad_squared * 2.0 * linear).astype(jnp.bfloat16)
    factor = float(TOKENS) ** -0.5
    grad_down_t = jnp.dot(out_grad.T, squared, preferred_element_type=jnp.float32) * factor
    grad_up = jnp.dot(inputs.T, grad_pre, preferred_element_type=jnp.float32) * factor
    blocks = N_FS * N_TP
    width = FF // blocks
    total = jnp.zeros((inputs.shape[0], D), jnp.float32)
    for index in range(blocks):
        term = jnp.dot(grad_pre[:, index * width:(index + 1) * width], w_up[:, index * width:(index + 1) * width].T, preferred_element_type=jnp.float32)
        term = lax.optimization_barrier(term.astype(jnp.bfloat16))
        total = total + term.astype(jnp.float32)
    return total.astype(jnp.bfloat16), grad_up, grad_down_t
```

```python
import functools

import jax
import jax.numpy as jnp
from jax import lax
from jax.experimental import pallas as pl
from jax.experimental.pallas import tpu as pltpu
from jax.sharding import PartitionSpec as P

BF16 = jnp.bfloat16
F32 = jnp.float32


def kernel(
    n, n_fs, chunks, factor,
    x_ref, og_ref, pre_ref, wu_ref, wd_ref,
    gin_ref, gu_ref, gd_ref,
    x_all, og_all, wu_all, wd_all, sq, gp, rs, tbuf, prec, frec,
    zs, zr, xs, xr, cs, cr, ts, tr, fsend, frecv,
):
    r, f, t = lax.axis_index("rep"), lax.axis_index("fs"), lax.axis_index("tp")
    tok, d_model = og_ref.shape
    shard, cols = wd_ref.shape
    crow = shard // chunks
    partner = {"tp": 1 - t}
    peers = [None] + [{"fs": lax.rem(f + d, n_fs)} for d in range(1, n_fs)]
    ahead = ({"rep": lax.rem(r + 1, n)}, {"rep": lax.rem(r + n - 1, n)})
    depth = (r, n - 1 - r)
    has_prev = (r > 0, r < n - 1)
    has_next = (r < n - 1, r > 0)

    barrier = pltpu.get_barrier_semaphore()
    for way in range(2):
        @pl.when(has_next[way])
        def _(way=way):
            pl.semaphore_signal(barrier, inc=1, device_id=ahead[way])
    for d in range(1, n_fs):
        pl.semaphore_signal(barrier, inc=1, device_id=peers[d])
    pl.semaphore_signal(barrier, inc=1, device_id=partner)
    pl.semaphore_wait(
        barrier, n_fs + jnp.where(r > 0, 1, 0) + jnp.where(r < n - 1, 1, 0)
    )

    def remote(src, dst, send, recv, target):
        return pltpu.make_async_remote_copy(
            src_ref=src, dst_ref=dst, send_sem=send, recv_sem=recv,
            device_id=target, device_id_type=pl.DeviceIdType.MESH,
        )

    def rows_of(ref, ff, tt):
        return ref.at[pl.ds(pl.multiple_of((ff * 2 + tt) * tok, tok), tok), :]

    def z_copy(phase, way, k, j, src, dst):
        return remote(
            src, dst, zs.at[phase, way, k, j], zr.at[phase, way, k, j], ahead[way]
        )

    def piece(ref, j):
        return ref.at[pl.ds(pl.multiple_of(j * crow, crow), crow), :]

    def send_own(phase, own, everyone):
        for way in range(2):
            @pl.when(has_next[way])
            def _(way=way):
                for j in range(chunks):
                    z_copy(
                        phase, way, 0, j, piece(own, j), piece(everyone.at[r], j)
                    ).start()

    def spread_start(q, own, everyone):
        for d in range(1, n_fs):
            remote(
                own, rows_of(everyone, f, t), xs.at[q, d], xr.at[q, d], peers[d]
            ).start()
        remote(
            own, rows_of(everyone, f, t), cs.at[q, 0], cr.at[q, 0], partner
        ).start()
        everyone[pl.ds(pl.multiple_of((f * 2 + t) * tok, tok), tok), :] = own[...]

    def spread_pass(q, everyone):
        for d in range(1, n_fs):
            src = rows_of(everyone, lax.rem(f + n_fs - d, n_fs), t)
            remote(src, src, xs.at[q, d], xr.at[q, d], peers[d]).wait()
            remote(src, src, cs.at[q, d], cr.at[q, d], partner).start()

    def spread_end(q, everyone):
        for d in range(n_fs):
            there = rows_of(everyone, lax.rem(f + n_fs - d, n_fs), 1 - t)
            remote(there, there, cs.at[q, d], cr.at[q, d], partner).wait()

    spread_start(0, og_ref, og_all)
    send_own(0, wd_ref, wd_all)
    wd_all[r] = wd_ref[...]
    wu_all[r] = wu_ref[...]
    tile = 2 * tok

    def square(i, _):
        at = pl.ds(pl.multiple_of(i * tile, tile), tile)
        linear = jnp.maximum(pre_ref[at, :].astype(F32), 0.0)
        sq[at, :] = (linear * linear).astype(BF16)
        return 0

    lax.fori_loop(0, n_fs, square, 0)
    spread_pass(0, og_all)
    spread_end(0, og_all)
    spread_start(1, x_ref, x_all)

    def partial(left, right, s, j):
        at = pl.ds(pl.multiple_of(s * shard + j * crow, crow), crow)
        return lax.dot_general(
            left[:, at], right[...], (((0,), (0,)), ((), ())),
            preferred_element_type=F32,
        ) * factor

    def one_round(phase, everyone, left, right, k):
        def one_piece(j, _):
            at = pl.ds(pl.multiple_of(j * crow, crow), crow)
            for way in range(2):
                sign = 1 - 2 * way
                slots = rs.at[phase, way]

                @pl.when(k < depth[way])
                def _(way=way, sign=sign):
                    block = piece(everyone.at[r - sign * (1 + k)], j)
                    z_copy(phase, way, k, j, block, block).wait_recv()

                    @pl.when(has_next[way])
                    def _():
                        z_copy(phase, way, k + 1, j, block, block).start()

                @pl.when(k >= depth[way])
                def _(way=way, slots=slots):
                    back = k - depth[way]
                    s = n - 1 - back if way == 0 else back
                    term = partial(left, right, s, j)
                    block = piece(slots.at[s], j)

                    @pl.when(has_prev[way])
                    def _():
                        z_copy(phase, way, k, j, block, block).wait_recv()
                        slots[s, at, :] = (term + slots[s, at, :].astype(F32)).astype(BF16)

                    @pl.when(jnp.logical_not(has_prev[way]))
                    def _():
                        slots[s, at, :] = term.astype(BF16)

                    z_copy(phase, way, k + 1, j, block, block).start()
            return 0

        lax.fori_loop(0, chunks, one_piece, 0)

    def last_round(phase, left, right, out):
        def one_piece(j, _):
            at = pl.ds(pl.multiple_of(j * crow, crow), crow)
            out[at, :] = partial(left, right, r, j)
            for way in range(2):
                @pl.when(has_prev[way])
                def _(way=way):
                    block = piece(rs.at[phase, way, r], j)
                    z_copy(phase, way, n - 1, j, block, block).wait_recv()
                    out[at, :] += rs[phase, way, r, at, :].astype(F32)
            return 0

        lax.fori_loop(0, chunks, one_piece, 0)

    def round_down(k, _):
        one_round(0, wd_all, og_all, sq, k)
        return 0

    lax.fori_loop(0, n - 1, round_down, 0)
    send_own(1, wu_ref, wu_all)
    spread_pass(1, x_all)

    def make_grad_pre(i, _):
        at = pl.ds(pl.multiple_of(i * tile, tile), tile)
        total = jnp.zeros((tile, cols), F32)
        for s in range(n):
            total += jnp.dot(
                og_all[at, s * shard:(s + 1) * shard], wd_all[s],
                preferred_element_type=F32,
            )
        linear = jnp.maximum(pre_ref[at, :].astype(F32), 0.0)
        gp[at, :] = (total * 2.0 * linear).astype(BF16)
        return 0

    lax.fori_loop(0, n_fs, make_grad_pre, 0)
    spread_end(1, x_all)
    last_round(0, og_all, sq, gd_ref)

    def cross(s):
        return remote(tbuf.at[s, 1 - t], prec.at[s], ts.at[s], tr.at[s], partner)

    def out_copy(s, d):
        rows = pl.ds(pl.multiple_of(lax.rem(f + d, n_fs) * tok, tok), tok)
        return remote(
            prec.at[s, rows, :], frec.at[s, d - 1],
            fsend.at[s, d], frecv.at[s, d], peers[d],
        )

    def block_term(s):
        def body(i, _):
            at = pl.ds(pl.multiple_of(i * tile, tile), tile)
            here = pl.ds(pl.multiple_of(i * tok, tok), tok)
            term = lax.dot_general(
                gp[at, :], wu_all[s], (((1,), (1,)), ((), ())),
                preferred_element_type=F32,
            ).astype(BF16)
            tbuf[s, 0, here, :] = term[:tok]
            tbuf[s, 1, here, :] = term[tok:]
            return 0

        lax.fori_loop(0, n_fs, body, 0)
        cross(s).start()

    def chip_sum(s):
        cross(s).wait()

        def body(i, _):
            here = pl.ds(pl.multiple_of(i * tok, tok), tok)
            prec[s, here, :] = (
                prec[s, here, :].astype(F32) + tbuf[s, t, here, :].astype(F32)
            ).astype(BF16)
            return 0

        lax.fori_loop(0, n_fs, body, 0)
        for d in range(1, n_fs):
            out_copy(s, d).start()

    def for_new(k, work):
        def body(way, _):
            @pl.when(jnp.where(way == 0, k < r, k < n - 1 - r))
            def _():
                work(jnp.where(way == 0, r - 1 - k, r + 1 + k))
            return 0

        lax.fori_loop(0, 2, body, 0)

    block_term(r)

    def round_up(k, _):
        one_round(1, wu_all, x_all, gp, k)
        for_new(k, block_term)

        @pl.when(k == 0)
        def _():
            chip_sum(r)

        @pl.when(k > 0)
        def _():
            for_new(k - 1, chip_sum)
        return 0

    lax.fori_loop(0, n - 1, round_up, 0)
    for_new(n - 2, chip_sum)
    last_round(1, x_all, gp, gu_ref)

    own_rows = pl.ds(pl.multiple_of(f * tok, tok), tok)
    for s in range(n):
        total = prec[s, own_rows, :].astype(F32)
        for d in range(1, n_fs):
            out_copy(s, d).wait()
            total += frec[s, d - 1].astype(F32)
        gin_ref[:, s * shard:(s + 1) * shard] = total.astype(BF16)

    for way in range(2):
        @pl.when(has_next[way])
        def _(way=way):
            def body(k, _):
                for phase in range(2):
                    for j in range(chunks):
                        block = piece(rs.at[0, 0, 0], j)
                        z_copy(phase, way, k, j, block, block).wait_send()
                return 0

            lax.fori_loop(0, n, body, 0)


def on_device(n, n_fs, inputs, out_grad, pre_act, w_up, w_down_t):
    tok, d_model = inputs.shape
    group, cols = pre_act.shape
    shard = w_up.shape[0]
    chunks = max(1, shard // 128)
    factor = float(group * n) ** -0.5
    dma = pltpu.SemaphoreType.DMA
    vmem = pl.BlockSpec(memory_space=pltpu.VMEM)
    grad_in, grad_up, grad_down_t = pl.pallas_call(
        functools.partial(kernel, n, n_fs, chunks, factor),
        out_shape=(
            jax.ShapeDtypeStruct((tok, d_model), BF16),
            jax.ShapeDtypeStruct((shard, cols), F32),
            jax.ShapeDtypeStruct((shard, cols), F32),
        ),
        in_specs=[vmem] * 5,
        out_specs=(vmem,) * 3,
        scratch_shapes=[
            pltpu.VMEM((group, d_model), BF16),
            pltpu.VMEM((group, d_model), BF16),
            pltpu.VMEM((n, shard, cols), BF16),
            pltpu.VMEM((n, shard, cols), BF16),
            pltpu.VMEM((group, cols), BF16),
            pltpu.VMEM((group, cols), BF16),
            pltpu.VMEM((2, 2, n, shard, cols), BF16),
            pltpu.VMEM((n, 2, n_fs * tok, shard), BF16),
            pltpu.VMEM((n, n_fs * tok, shard), BF16),
            pltpu.VMEM((n, n_fs - 1, tok, shard), BF16),
            dma((2, 2, n, chunks)),
            dma((2, 2, n, chunks)),
            dma((2, n_fs)),
            dma((2, n_fs)),
            dma((2, n_fs)),
            dma((2, n_fs)),
            dma((n,)),
            dma((n,)),
            dma((n, n_fs)),
            dma((n, n_fs)),
        ],
        compiler_params=pltpu.CompilerParams(
            collective_id=0, has_side_effects=True, vmem_limit_bytes=67043328
        ),
    )(inputs, out_grad, pre_act, w_up, w_down_t)
    return grad_in, grad_up, grad_down_t


def solution(mesh):
    rows = P(("rep", "fs", "tp"), None)
    blocks = P("rep", ("fs", "tp"))
    return jax.shard_map(
        functools.partial(on_device, mesh.shape["rep"], mesh.shape["fs"]),
        mesh=mesh,
        in_specs=(rows, rows, blocks, blocks, blocks),
        out_specs=(rows, blocks, blocks),
        check_vma=False,
    )
```

```python
import functools

import jax
import jax.numpy as jnp
from jax import lax
from jax.experimental import pallas as pl
from jax.experimental.pallas import tpu as pltpu
from jax.sharding import PartitionSpec as P

BF16 = jnp.bfloat16
F32 = jnp.float32


def kernel(
    n, n_fs, chunks, factor,
    x_ref, og_ref, pre_ref, wu_ref, wd_ref,
    gin_ref, gu_ref, gd_ref,
    x_all, og_all, wu_all, wd_all, sq, gp, rs, tbuf, prec, frec,
    pre, total, zs, zr, xs, xr, cs, cr, ts, tr, fsend, frecv, ls,
):
    r, f, t = lax.axis_index("rep"), lax.axis_index("fs"), lax.axis_index("tp")
    tok, d_model = og_ref.shape
    shard, cols = wd_ref.shape
    crow = shard // chunks
    partner = {"tp": 1 - t}
    own_tokens = pl.ds(pl.multiple_of((f * 2 + t) * tok, tok), tok)
    loads = [
        pltpu.make_async_copy(src, dst, ls.at[i])
        for i, (src, dst) in enumerate((
            (pre_ref, pre),
            (og_ref, og_all.at[own_tokens, :]),
            (x_ref, x_all.at[own_tokens, :]),
            (wd_ref, wd_all.at[r]),
            (wu_ref, wu_all.at[r]),
        ))
    ]
    peers = [None] + [{"fs": lax.rem(f + d, n_fs)} for d in range(1, n_fs)]
    ahead = ({"rep": lax.rem(r + 1, n)}, {"rep": lax.rem(r + n - 1, n)})
    depth = (r, n - 1 - r)
    has_prev = (r > 0, r < n - 1)
    has_next = (r < n - 1, r > 0)

    barrier = pltpu.get_barrier_semaphore()
    for way in range(2):
        @pl.when(has_next[way])
        def _(way=way):
            pl.semaphore_signal(barrier, inc=1, device_id=ahead[way])
    for d in range(1, n_fs):
        pl.semaphore_signal(barrier, inc=1, device_id=peers[d])
    pl.semaphore_signal(barrier, inc=1, device_id=partner)
    pl.semaphore_wait(
        barrier, n_fs + jnp.where(r > 0, 1, 0) + jnp.where(r < n - 1, 1, 0)
    )

    def remote(src, dst, send, recv, target):
        return pltpu.make_async_remote_copy(
            src_ref=src, dst_ref=dst, send_sem=send, recv_sem=recv,
            device_id=target, device_id_type=pl.DeviceIdType.MESH,
        )

    def rows_of(ref, ff, tt):
        return ref.at[pl.ds(pl.multiple_of((ff * 2 + tt) * tok, tok), tok), :]

    def z_copy(phase, way, k, j, src, dst):
        return remote(
            src, dst, zs.at[phase, way, k, j], zr.at[phase, way, k, j], ahead[way]
        )

    def piece(ref, j):
        return ref.at[pl.ds(pl.multiple_of(j * crow, crow), crow), :]

    def send_own(phase, own, everyone, when):
        for way in range(2):
            @pl.when(jnp.logical_and(has_next[way], when[way]))
            def _(way=way):
                for j in range(chunks):
                    z_copy(
                        phase, way, 0, j, piece(own, j), piece(everyone.at[r], j)
                    ).start()

    def spread_start(q, own, everyone):
        for d in range(1, n_fs):
            remote(
                own, rows_of(everyone, f, t), xs.at[q, d], xr.at[q, d], peers[d]
            ).start()
        remote(
            own, rows_of(everyone, f, t), cs.at[q, 0], cr.at[q, 0], partner
        ).start()

    def spread_pass(q, everyone):
        for d in range(1, n_fs):
            src = rows_of(everyone, lax.rem(f + n_fs - d, n_fs), t)
            remote(src, src, xs.at[q, d], xr.at[q, d], peers[d]).wait()
            remote(src, src, cs.at[q, d], cr.at[q, d], partner).start()

    def spread_end(q, everyone):
        for d in range(n_fs):
            there = rows_of(everyone, lax.rem(f + n_fs - d, n_fs), 1 - t)
            remote(there, there, cs.at[q, d], cr.at[q, d], partner).wait()

    send_own(0, wd_ref, wd_all, (True, True))
    spread_start(0, og_ref, og_all)
    send_own(1, wu_ref, wu_all, (depth[0] == 0, depth[1] == 0))
    for load in loads:
        load.start()
    for load in loads:
        load.wait()
    tile = 2 * tok

    def square(i, _):
        at = pl.ds(pl.multiple_of(i * tile, tile), tile)
        linear = jnp.maximum(pre[at, :].astype(F32), 0.0)
        sq[at, :] = (linear * linear).astype(BF16)
        return 0

    lax.fori_loop(0, n_fs, square, 0)
    spread_pass(0, og_all)
    spread_end(0, og_all)
    spread_start(1, x_ref, x_all)

    def partial(left, right, s, j):
        at = pl.ds(pl.multiple_of(s * shard + j * crow, crow), crow)
        return lax.dot_general(
            left[:, at], right[...], (((0,), (0,)), ((), ())),
            preferred_element_type=F32,
        ) * factor

    def one_round(phase, everyone, left, right, k):
        def one_piece(j, _):
            at = pl.ds(pl.multiple_of(j * crow, crow), crow)
            for way in range(2):
                sign = 1 - 2 * way
                slots = rs.at[phase, way]

                @pl.when(k < depth[way])
                def _(way=way, sign=sign):
                    block = piece(everyone.at[r - sign * (1 + k)], j)
                    z_copy(phase, way, k, j, block, block).wait_recv()

                    @pl.when(has_next[way])
                    def _():
                        z_copy(phase, way, k + 1, j, block, block).start()

                @pl.when(k >= depth[way])
                def _(way=way, slots=slots):
                    back = k - depth[way]
                    s = n - 1 - back if way == 0 else back
                    term = partial(left, right, s, j)
                    block = piece(slots.at[s], j)

                    @pl.when(has_prev[way])
                    def _():
                        z_copy(phase, way, k, j, block, block).wait_recv()
                        slots[s, at, :] = (term + slots[s, at, :].astype(F32)).astype(BF16)

                    @pl.when(jnp.logical_not(has_prev[way]))
                    def _():
                        slots[s, at, :] = term.astype(BF16)

                    z_copy(phase, way, k + 1, j, block, block).start()
            return 0

        lax.fori_loop(0, chunks, one_piece, 0)

    def last_round(phase, left, right, out, low, high):
        def one_piece(j, _):
            at = pl.ds(pl.multiple_of(j * crow, crow), crow)
            total[...] = partial(left, right, r, j)
            for way in range(2):
                @pl.when(has_prev[way])
                def _(way=way):
                    block = piece(rs.at[phase, way, r], j)
                    z_copy(phase, way, n - 1, j, block, block).wait_recv()
                    total[...] += rs[phase, way, r, at, :].astype(F32)
            out[at, :] = total[...].astype(BF16)
            return 0

        lax.fori_loop(low, high, one_piece, 0)

    def round_down(k, _):
        one_round(0, wd_all, og_all, sq, k)
        send_own(1, wu_ref, wu_all, (depth[0] == k + 1, depth[1] == k + 1))
        return 0

    lax.fori_loop(0, n - 1, round_down, 0)
    spread_pass(1, x_all)

    def make_grad_pre(i, _):
        at = pl.ds(pl.multiple_of(i * tile, tile), tile)
        acc = jnp.zeros((tile, cols), F32)
        for s in range(n):
            acc += jnp.dot(
                og_all[at, s * shard:(s + 1) * shard], wd_all[s],
                preferred_element_type=F32,
            )
        linear = jnp.maximum(pre[at, :].astype(F32), 0.0)
        gp[at, :] = (acc * 2.0 * linear).astype(BF16)
        return 0

    lax.fori_loop(0, n_fs, make_grad_pre, 0)
    spread_end(1, x_all)

    def cross(s):
        return remote(tbuf.at[s, 1 - t], prec.at[s], ts.at[s], tr.at[s], partner)

    def out_copy(s, d):
        rows = pl.ds(pl.multiple_of(lax.rem(f + d, n_fs) * tok, tok), tok)
        return remote(
            prec.at[s, rows, :], frec.at[s, d - 1],
            fsend.at[s, d], frecv.at[s, d], peers[d],
        )

    def block_term(s):
        def body(i, _):
            at = pl.ds(pl.multiple_of(i * tile, tile), tile)
            here = pl.ds(pl.multiple_of(i * tok, tok), tok)
            term = lax.dot_general(
                gp[at, :], wu_all[s], (((1,), (1,)), ((), ())),
                preferred_element_type=F32,
            ).astype(BF16)
            tbuf[s, 0, here, :] = term[:tok]
            tbuf[s, 1, here, :] = term[tok:]
            return 0

        lax.fori_loop(0, n_fs, body, 0)
        cross(s).start()

    def chip_sum(s):
        cross(s).wait()

        def body(i, _):
            here = pl.ds(pl.multiple_of(i * tok, tok), tok)
            prec[s, here, :] = (
                prec[s, here, :].astype(F32) + tbuf[s, t, here, :].astype(F32)
            ).astype(BF16)
            return 0

        lax.fori_loop(0, n_fs, body, 0)
        for d in range(1, n_fs):
            out_copy(s, d).start()

    def for_new(k, work):
        def body(way, _):
            @pl.when(jnp.where(way == 0, k < r, k < n - 1 - r))
            def _():
                work(jnp.where(way == 0, r - 1 - k, r + 1 + k))
            return 0

        lax.fori_loop(0, 2, body, 0)

    one_round(1, wu_all, x_all, gp, 0)
    block_term(r)
    for_new(0, block_term)
    last_round(0, og_all, sq, gd_ref, 0, chunks)
    chip_sum(r)

    def round_up(k, _):
        one_round(1, wu_all, x_all, gp, k)
        for_new(k, block_term)
        for_new(k - 1, chip_sum)
        return 0

    lax.fori_loop(1, n - 1, round_up, 0)
    for_new(n - 2, chip_sum)
    last_round(1, x_all, gp, gu_ref, 0, chunks - 1)

    own_rows = pl.ds(pl.multiple_of(f * tok, tok), tok)
    for s in range(n):
        acc = prec[s, own_rows, :].astype(F32)
        for d in range(1, n_fs):
            out_copy(s, d).wait()
            acc += frec[s, d - 1].astype(F32)
        gin_ref[:, s * shard:(s + 1) * shard] = acc.astype(BF16)
    last_round(1, x_all, gp, gu_ref, chunks - 1, chunks)

    for way in range(2):
        @pl.when(has_next[way])
        def _(way=way):
            def body(k, _):
                for phase in range(2):
                    for j in range(chunks):
                        block = piece(rs.at[0, 0, 0], j)
                        z_copy(phase, way, k, j, block, block).wait_send()
                return 0

            lax.fori_loop(0, n, body, 0)


def on_device(n, n_fs, inputs, out_grad, pre_act, w_up, w_down_t):
    tok, d_model = inputs.shape
    group, cols = pre_act.shape
    shard = w_up.shape[0]
    chunks = max(1, shard // 128)
    factor = float(group * n) ** -0.5
    dma = pltpu.SemaphoreType.DMA
    vmem = pl.BlockSpec(memory_space=pltpu.VMEM)
    grad_in, grad_up, grad_down_t = pl.pallas_call(
        functools.partial(kernel, n, n_fs, chunks, factor),
        out_shape=(
            jax.ShapeDtypeStruct((tok, d_model), BF16),
            jax.ShapeDtypeStruct((shard, cols), BF16),
            jax.ShapeDtypeStruct((shard, cols), BF16),
        ),
        in_specs=[pl.BlockSpec(memory_space=pl.ANY)] * 5,
        out_specs=(vmem,) * 3,
        scratch_shapes=[
            pltpu.VMEM((group, d_model), BF16),
            pltpu.VMEM((group, d_model), BF16),
            pltpu.VMEM((n, shard, cols), BF16),
            pltpu.VMEM((n, shard, cols), BF16),
            pltpu.VMEM((group, cols), BF16),
            pltpu.VMEM((group, cols), BF16),
            pltpu.VMEM((2, 2, n, shard, cols), BF16),
            pltpu.VMEM((n, 2, n_fs * tok, shard), BF16),
            pltpu.VMEM((n, n_fs * tok, shard), BF16),
            pltpu.VMEM((n, n_fs - 1, tok, shard), BF16),
            pltpu.VMEM((group, cols), BF16),
            pltpu.VMEM((shard // chunks, cols), F32),
            dma((2, 2, n, chunks)),
            dma((2, 2, n, chunks)),
            dma((2, n_fs)),
            dma((2, n_fs)),
            dma((2, n_fs)),
            dma((2, n_fs)),
            dma((n,)),
            dma((n,)),
            dma((n, n_fs)),
            dma((n, n_fs)),
            dma((5,)),
        ],
        compiler_params=pltpu.CompilerParams(
            collective_id=0, has_side_effects=True, vmem_limit_bytes=67043328
        ),
    )(inputs, out_grad, pre_act, w_up, w_down_t)
    return grad_in, grad_up.astype(F32), grad_down_t.astype(F32)


def solution(mesh):
    rows = P(("rep", "fs", "tp"), None)
    blocks = P("rep", ("fs", "tp"))
    return jax.shard_map(
        functools.partial(on_device, mesh.shape["rep"], mesh.shape["fs"]),
        mesh=mesh,
        in_specs=(rows, rows, blocks, blocks, blocks),
        out_specs=(rows, blocks, blocks),
        check_vma=False,
    )
```
